32 devices in a mesh: ep: 16 (over z, y, x), tp: 2 (over core).
Axes of the slice: x: 2, y: 2, z: 4, core: 2. Of those that a mesh axis runs over, the one named last changes fastest.
Arguments:
- tokens: bfloat16 [384, 2048], P('ep'), may hold values from -40 to 40
- old_state: float32 [384, 16, 4096], P('ep', 'tp'), may hold values from -6 to 6
- w_query: bfloat16 [2048, 1024], P(None, 'tp'), may hold values from -0.125 to 0.125
- w_forget: bfloat16 [2048, 1024], P(None, 'tp'), may hold values from -0.125 to 0.125
- w_value: bfloat16 [2048, 1024], P(None, 'tp'), may hold values from -0.125 to 0.125
- w_gate: bfloat16 [2048, 1024], P(None, 'tp'), may hold values from -0.125 to 0.125
- lower_bound: float32 [1024], P('tp'), may hold values from 0.05 to 0.9
- head_gain: float32 [64], replicated, may hold values from 0.1 to 1.9
- w_out: bfloat16 [1024, 2048], P('tp'), may hold values from -0.1875 to 0.1875
- mix_gain: float32 [2048], replicated, may hold values from 0.1 to 1.9
- expert_gate: bfloat16 [16, 2048, 512], P('ep', None, 'tp'), may hold values from -0.125 to 0.125
- expert_up: bfloat16 [16, 2048, 512], P('ep', None, 'tp'), may hold values from -0.125 to 0.125
- expert_down: bfloat16 [16, 512, 2048], P('ep', 'tp'), may hold values from -0.25 to 0.25
- expert_ids: int32 [384, 2], P('ep'), may hold values from 0 to 15, as said below
- route_weight: float32 [384, 2], P('ep'), may hold values from 0.1 to 1
- moe_gain: float32 [2048], replicated, may hold values from 0.1 to 1.9
Outputs:
- next_tokens: bfloat16 [384, 2048], P('ep', 'tp')
- new_state: float32 [384, 16, 4096], P('ep', 'tp')
The draws below stay inside these ranges and needn't reach their ends.
Inputs may be any that keep to these rules, and one draw needn't show every extreme that they name: `expert_ids`: each row names two different experts of one group of 4 consecutive experts. In each aligned block of 24 rows no expert is named by more than 6 rows, and one expert, the same in every block, is named by exactly 6 rows of every block.
All inputs are finite; a program needn't handle non-finite values.
Results may differ from the reference program's by a relative error of at most 0.011.
Values may be sent and summed in bfloat16 or wider, within the bound.
A program may use at most 128 MiB of HBM per device.

```python
import math
import jax
import jax.numpy as jnp
from jax import lax

D = 2048
HEADS = 16
HD = 64
FF = 512
EPG = 4
TOPK = 2
SEQ_DEV = 24
HW = 1024
SEQS = 384
EXPERTS = 16
GROUPS = 4
CAP = 6
N_TP = 2


def draw_tokens(key, part):
    draw_keys = jax.random.split(key, 4)
    column_scale = jnp.exp(jax.random.uniform(draw_keys[0], (D,), jnp.float32, 0.0, math.log(10.0)))
    column_scale = column_scale / jnp.sqrt(jnp.mean(column_scale * column_scale))
    row_scale = jnp.exp(jax.random.uniform(draw_keys[1], (SEQS, 1), jnp.float32, math.log(0.5), math.log(2.0)))
    noise = jax.random.normal(draw_keys[3], (SEQS, D), jnp.float32)
    noise = jnp.clip(noise, -6.0, 6.0)
    return (noise * column_scale[None, :] * row_scale).astype(jnp.bfloat16)


def draw_expert_ids(key, part):
    block_count = SEQS // SEQ_DEV
    lane_count = GROUPS * 2 * CAP
    popular = jax.random.randint(jax.random.fold_in(key, 1), (GROUPS,), 1, 9)
    forced_group = jax.random.randint(jax.random.fold_in(key, 2), (), 0, GROUPS)
    base_scores = jax.random.randint(jax.random.fold_in(key, 3), (EPG,), 0, 1024) * EPG + jnp.arange(EPG)
    base_order = jnp.argsort(base_scores, stable=True)

    def one_block(block_key):
        block_keys = jax.random.split(block_key, 3)
        order_scores = jax.random.randint(block_keys[0], (GROUPS, EPG), 0, 1024) * EPG + jnp.arange(EPG)[None, :]
        orders = jnp.argsort(order_scores, axis=1, stable=True)
        orders = jnp.where((jnp.arange(GROUPS) == forced_group)[:, None], base_order[None, :], orders)
        lane_ids = jnp.arange(lane_count)
        lane_group = lane_ids // (2 * CAP)
        lane_pair = lane_ids % (2 * CAP) // CAP
        lane_score = jax.random.randint(block_keys[1], (lane_count,), 0, 16384) * popular[lane_group]
        forced = (lane_group == forced_group) & (lane_pair == 0)
        lane_rank = lane_score * 4096 + lane_ids + jnp.where(forced, 1 << 30, 0)
        chosen = lax.top_k(lane_rank.astype(jnp.int32), SEQ_DEV)[1]
        chosen = jax.random.permutation(block_keys[2], chosen)
        row_group = lane_group[chosen]
        row_pair = lane_pair[chosen]
        first_expert = orders[row_group, 2 * row_pair] + row_group * EPG
        second_expert = orders[row_group, 2 * row_pair + 1] + row_group * EPG
        return jnp.stack([first_expert, second_expert], 1)
    routed = jax.vmap(one_block)(jax.random.split(jax.random.fold_in(key, 4), block_count))
    return routed.reshape(SEQS, TOPK).astype(jnp.int32)


def level_of(stream_key, dims, cuts, least, high):
    def one(axis_at, shards_of):
        draws = jax.random.uniform(jax.random.fold_in(jax.random.fold_in(stream_key, 6), axis_at), (shards_of,), jnp.float32, least / len(cuts), high / len(cuts))
        return jnp.repeat(jnp.exp(draws), dims[axis_at] // shards_of).reshape((-1,) + (1,) * (len(dims) - axis_at - 1))

    level = one(*cuts[0])
    for cut in cuts[1:]:
        level = level * one(*cut)
    return level


def normal_values(key, extent, spread, most, cuts=(), held_as=jnp.bfloat16):
    factor_of = level_of(key, extent, cuts, -0.22, 0.18) if cuts else 1.0
    array = jax.random.normal(key, extent, jnp.float32) * spread * factor_of
    return jnp.minimum(jnp.maximum(array, -most), most).astype(held_as)


def setup_inputs(seed: int = 0) -> dict:
    arg_keys = jax.random.split(jax.random.key(seed), 17)
    return {
        "tokens": draw_tokens(jax.random.fold_in(arg_keys[16], 71), 0),
        "old_state": normal_values(arg_keys[1], (SEQS, HEADS, HD * HD), 1.0, 6.0, ((0, 16), (1, 2)), jnp.float32),
        "w_query": normal_values(arg_keys[2], (D, HW), D ** -0.5, 0.125, ((1, 2),)),
        "w_forget": normal_values(arg_keys[3], (D, HW), D ** -0.5, 0.125, ((1, 2),)),
        "w_value": normal_values(arg_keys[4], (D, HW), D ** -0.5, 0.125, ((1, 2),)),
        "w_gate": normal_values(arg_keys[5], (D, HW), D ** -0.5, 0.125, ((1, 2),)),
        "lower_bound": jnp.clip(0.05 + 0.84999998 * jax.random.uniform(arg_keys[6], (HW,), jnp.float32) ** level_of(arg_keys[6], (HW,), ((0, 2),), -0.2, 0.2), 0.05, 0.9),
        "head_gain": jnp.clip(1.0 + 0.18 * jax.random.normal(arg_keys[7], (HD,), jnp.float32), 0.1, 1.9),
        "w_out": normal_values(arg_keys[8], (HW, D), HW ** -0.5, 0.1875, ((0, 2),)),
        "mix_gain": jnp.clip(1.0 + 0.18 * jax.random.normal(arg_keys[9], (D,), jnp.float32), 0.1, 1.9),
        "expert_gate": normal_values(arg_keys[10], (EXPERTS, D, FF), D ** -0.5, 0.125, ((0, 16), (2, 2))),
        "expert_up": normal_values(arg_keys[11], (EXPERTS, D, FF), D ** -0.5, 0.125, ((0, 16), (2, 2))),
        "expert_down": normal_values(arg_keys[12], (EXPERTS, FF, D), FF ** -0.5, 0.25, ((0, 16), (1, 2))),
        "expert_ids": draw_expert_ids(jax.random.fold_in(arg_keys[16], 71), 0),
        "route_weight": jnp.clip(jnp.exp(math.log(1.0) - 2.3025851 * jax.random.uniform(arg_keys[14], (SEQS, TOPK), jnp.float32) ** level_of(arg_keys[14], (SEQS, TOPK), ((0, 16),), -0.2, 0.2)), 0.1, 1.0),
        "moe_gain": jnp.clip(1.0 + 0.18 * jax.random.normal(arg_keys[15], (D,), jnp.float32), 0.1, 1.9),
    }


def layer_normed(values, gain):
    center = lax.optimization_barrier(jnp.mean(values, -1, keepdims=True))
    centered = values - center
    variance = lax.optimization_barrier(jnp.mean(centered * centered, -1, keepdims=True))
    return centered * lax.rsqrt(variance + 1e-05) * gain

def rounded(values):
    return lax.optimization_barrier(values.astype(jnp.bfloat16)).astype(jnp.float32)

def slot_table(ids_block, expert_count, capacity):
    flat_ids = ids_block.reshape(-1)
    onehot = (flat_ids[:, None] == jnp.arange(expert_count, dtype=jnp.int32)[None, :]).astype(jnp.int32)
    before = jnp.cumsum(onehot, 0) - onehot
    rank = lax.optimization_barrier(jnp.sum(before * onehot, 1)).astype(jnp.int32)
    return (flat_ids * capacity + rank).astype(jnp.int32)

def reference(tokens, old_state, w_query, w_forget, w_value, w_gate, lower_bound, head_gain, w_out, mix_gain, expert_gate, expert_up, expert_down, expert_ids, route_weight, moe_gain):
    row_count = tokens.shape[0]
    half_cols = HW // N_TP
    q_lin = jnp.dot(tokens, w_query, preferred_element_type=jnp.float32)
    f_lin = jnp.dot(tokens, w_forget, preferred_element_type=jnp.float32)
    v_lin = jnp.dot(tokens, w_value, preferred_element_type=jnp.float32)
    g_lin = jnp.dot(tokens, w_gate, preferred_element_type=jnp.float32)
    act_query = jax.nn.silu(q_lin).reshape(row_count, HEADS, HD)
    bound = lower_bound.reshape(HEADS, HD)
    forget = bound + (1.0 - bound) * jax.nn.sigmoid(f_lin.reshape(row_count, HEADS, HD))
    previous = old_state.reshape(row_count, HEADS, HD, HD)
    new_state = forget[..., None] * previous + (1.0 - forget)[..., None] * v_lin.reshape(row_count, HEADS, 1, HD)
    readout = jnp.einsum('shi,shij->shj', act_query, new_state, precision=lax.Precision.HIGHEST)
    normed = readout * lax.rsqrt(lax.optimization_barrier(jnp.mean(readout * readout, -1, keepdims=True)) + 1e-06) * head_gain
    mixer_out = (normed * jax.nn.silu(g_lin.reshape(row_count, HEADS, HD))).reshape(row_count, HW).astype(jnp.bfloat16)
    mixed = jnp.zeros((row_count, D), jnp.float32)
    for half_index in range(N_TP):
        lower = half_index * half_cols
        mixed = mixed + rounded(jnp.dot(mixer_out[:, lower:lower + half_cols], w_out[lower:lower + half_cols], preferred_element_type=jnp.float32))
    after_mixer = layer_normed(tokens.astype(jnp.float32) + mixed, mix_gain).astype(jnp.bfloat16)
    block_count = row_count // SEQ_DEV
    slot_count = EXPERTS * CAP
    id_blocks = expert_ids.reshape(block_count, SEQ_DEV, TOPK)
    slot_ids = jax.vmap(lambda one_block: slot_table(one_block, EXPERTS, CAP))(id_blocks)
    placing = (slot_ids[:, None, :] == jnp.arange(slot_count, dtype=jnp.int32)[None, :, None]).astype(jnp.float32)
    choose = placing.reshape(block_count, slot_count, SEQ_DEV, TOPK).sum(-1)
    row_blocks = after_mixer.reshape(block_count, SEQ_DEV, D).astype(jnp.float32)
    buffer = jnp.einsum('bcs,bsd->bcd', choose, row_blocks, precision=lax.Precision.HIGHEST).astype(jnp.bfloat16)
    by_expert = buffer.reshape(block_count, EXPERTS, CAP, D).transpose(1, 0, 2, 3).reshape(EXPERTS, block_count * CAP, D)
    half_units = FF // N_TP

    def run_expert(inputs):
        rows_in, gate_weight, up_weight, down_weight = inputs
        gate_act = jnp.dot(rows_in, gate_weight, preferred_element_type=jnp.float32)
        up_act = jnp.dot(rows_in, up_weight, preferred_element_type=jnp.float32)
        hidden = (jax.nn.silu(gate_act) * up_act).astype(jnp.bfloat16)
        total = jnp.zeros((rows_in.shape[0], D), jnp.float32)
        for half_index in range(N_TP):
            lower = half_index * half_units
            total = total + rounded(jnp.dot(hidden[:, lower:lower + half_units], down_weight[lower:lower + half_units], preferred_element_type=jnp.float32))
        return total.astype(jnp.bfloat16)
    results = lax.map(run_expert, (by_expert, expert_gate, expert_up, expert_down))
    returned = results.reshape(EXPERTS, block_count, CAP, D).transpose(1, 0, 2, 3).reshape(block_count, slot_count, D)
    picked = jnp.take_along_axis(returned, slot_ids[:, :, None], axis=1)
    picked = picked.reshape(row_count, TOPK, D).astype(jnp.float32)
    moe_sum = lax.optimization_barrier(jnp.sum(picked * route_weight[..., None], 1))
    next_tokens = layer_normed(after_mixer.astype(jnp.float32) + moe_sum, moe_gain).astype(jnp.bfloat16)
    return (next_tokens, new_state.reshape(row_count, HEADS, HD * HD))
```

```python
import functools

import jax
import jax.numpy as jnp
from jax import lax
from jax.experimental import pallas as pl
from jax.experimental.pallas import tpu as pltpu
from jax.sharding import PartitionSpec as P

F32 = jnp.float32
BF16 = jnp.bfloat16
MESH = pl.DeviceIdType.MESH


def silu(values):
    return values * jax.nn.sigmoid(values)


def mixer_kernel(
    tok, lb, hg, st_hbm, wq_hbm, wf_hbm, wv_hbm, wg_hbm, wo_hbm,
    ns_hbm, part,
    wq, wf, wv, wg, wo, st, ns, spread, qs, fs, vs, ro, mix, sems, out_sems,
):
    rows, heads, width = st.shape
    hd = hg.shape[1]
    loads = [
        pltpu.make_async_copy(src, dst, sems.at[at])
        for at, (src, dst) in enumerate(
            ((wf_hbm, wf), (wv_hbm, wv), (wq_hbm, wq), (st_hbm, st), (wg_hbm, wg), (wo_hbm, wo))
        )
    ]
    for load in loads:
        load.start()
    key_of = lax.broadcasted_iota(jnp.int32, spread.shape, 0) % hd
    lane_key = lax.broadcasted_iota(jnp.int32, spread.shape, 1) // hd
    spread[...] = jnp.where(key_of == lane_key, 1.0, 0.0).astype(BF16)

    def split_heads(values, ref):
        high = values.astype(BF16).astype(F32)
        low = values - high
        for h in range(heads):
            at = slice(h * hd, (h + 1) * hd)
            ref[:, h, 0:hd] = high[:, at]
            ref[:, h, hd : 2 * hd] = low[:, at]

    tokens = tok[...]
    loads[0].wait()
    f_lin = jnp.dot(tokens, wf[...], preferred_element_type=F32)
    bound = lb[...]
    split_heads(bound + (1.0 - bound) * jax.nn.sigmoid(f_lin), fs)
    loads[1].wait()
    v_lin = jnp.dot(tokens, wv[...], preferred_element_type=F32)
    for h in range(heads):
        at = slice(h * hd, (h + 1) * hd)
        vs[:, h, 0:hd] = v_lin[:, at]
        vs[:, h, hd : 2 * hd] = v_lin[:, at]
    loads[2].wait()
    q_lin = jnp.dot(tokens, wq[...], preferred_element_type=F32)
    split_heads(silu(q_lin), qs)
    loads[3].wait()
    flat = (rows * heads, 2 * hd)
    keep = fs[...].reshape(flat).astype(BF16)
    ask = qs[...].reshape(flat).astype(BF16)
    value = vs[...]
    pair = 2 * hd
    block = 2 * pair
    chunks = out_sems.shape[0]
    per_chunk = width // chunks
    acc = jnp.zeros((rows, heads, pair), F32)
    stores = []
    for chunk in range(chunks):

        def step(i, acc, chunk=chunk):
            start = pl.multiple_of(chunk * per_chunk + i * block, block)
            ones = spread[:, pl.ds(start, block)]
            f_wide = jnp.dot(keep, ones, preferred_element_type=F32).reshape(rows, heads, block)
            q_wide = jnp.dot(ask, ones, preferred_element_type=F32).reshape(rows, heads, block)
            for half in range(2):
                lanes = pl.ds(pl.multiple_of(start + half * pair, pair), pair)
                cut = slice(half * pair, (half + 1) * pair)
                new = value + f_wide[:, :, cut] * (st[:, :, lanes] - value)
                ns[:, :, lanes] = new
                acc = acc + q_wide[:, :, cut] * new
            return acc

        acc = lax.fori_loop(0, per_chunk // block, step, acc)
        span = pl.ds(chunk * per_chunk, per_chunk)
        store = pltpu.make_async_copy(ns.at[:, :, span], ns_hbm.at[:, :, span], out_sems.at[chunk])
        store.start()
        stores.append(store)
    readout = acc[:, :, 0:hd] + acc[:, :, hd:pair]
    square = jnp.mean(readout * readout, -1, keepdims=True)
    ro[...] = readout * lax.rsqrt(square + 1e-06) * hg[...].reshape(1, 1, hd)
    for h in range(heads):
        mix[:, h * hd : (h + 1) * hd] = ro[:, h, :]
    loads[4].wait()
    g_lin = jnp.dot(tokens, wg[...], preferred_element_type=F32)
    mixer_out = (mix[...] * silu(g_lin)).astype(BF16)
    loads[5].wait()
    part[...] = jnp.dot(mixer_out, wo[...], preferred_element_type=F32).astype(BF16)
    for store in stores:
        store.wait()


def expert_kernel(
    capacity, n,
    part, tok, mix_gain, ids, route, moe_gain, eg_hbm, eu_hbm, ed_hbm,
    out,
    eg, eu, ed, part_in, am, outgoing, mine, theirs, down_out, down_in, results, back,
    stat_out, stat_in,
    w_sems, pair_sems, s1, r1, s2, r2, fs, fr, ds_, dr,
):
    e = lax.axis_index("ep")
    c = lax.axis_index("tp")
    other = 1 - c
    rows, width = tok.shape
    slots = outgoing.shape[1]
    half = width // 2
    total = n * slots
    barrier = pltpu.get_barrier_semaphore()
    pl.semaphore_signal(barrier, inc=1, device_id=(e, other), device_id_type=MESH)
    for d in range(1, n):
        pl.semaphore_signal(barrier, inc=1, device_id=(lax.rem(e + d, n), c), device_id_type=MESH)
    loads = [
        pltpu.make_async_copy(src, dst, w_sems.at[at])
        for at, (src, dst) in enumerate(((eg_hbm, eg), (eu_hbm, eu), (ed_hbm, ed)))
    ]
    for load in loads:
        load.start()

    def remote(src, dst, send, recv, device):
        return pltpu.make_async_remote_copy(
            src_ref=src, dst_ref=dst, send_sem=send, recv_sem=recv,
            device_id=device, device_id_type=MESH,
        )

    lane = lax.broadcasted_iota(jnp.int32, (rows, total), 1)
    lane_expert = lane // slots
    lane_rank = (lane % slots).astype(F32)
    first = jnp.where(ids[:, 0:1] == lane_expert, 1.0, 0.0)
    second = jnp.where(ids[:, 1:2] == lane_expert, 1.0, 0.0)
    named = first + second
    row_at = lax.broadcasted_iota(jnp.int32, (rows, rows), 0)
    col_at = lax.broadcasted_iota(jnp.int32, (rows, rows), 1)
    earlier = jnp.where(col_at < row_at, 1.0, 0.0).astype(BF16)
    before = jnp.dot(earlier, named.astype(BF16), preferred_element_type=F32)
    place = jnp.where(before == lane_rank, named, 0.0)
    weigh = place * (first * route[:, 0:1] + second * route[:, 1:2])
    weigh_high = weigh.astype(BF16)
    weigh_low = (weigh - weigh_high.astype(F32)).astype(BF16)
    place_t = jnp.transpose(place).astype(BF16)

    pl.semaphore_wait(barrier, n)
    swap = remote(part, part_in, pair_sems.at[0], pair_sems.at[1], (e, other))
    swap.start()
    base = tok[...].astype(F32) + part[...].astype(F32)
    swap.wait()
    values = base + part_in[...].astype(F32)
    centered = values - jnp.mean(values, -1, keepdims=True)
    variance = jnp.mean(centered * centered, -1, keepdims=True)
    am[...] = centered * lax.rsqrt(variance + 1e-05) * mix_gain[...]

    own_cols = pl.ds(pl.multiple_of(c * half, half), half)
    other_cols = pl.ds(pl.multiple_of(other * half, half), half)
    am_half = am[:, own_cols].astype(BF16)
    sent = jnp.dot(place_t, am_half, preferred_element_type=F32)
    for at in range(n):
        outgoing[at] = sent[at * slots : (at + 1) * slots].astype(BF16)
    sends = []
    for d in range(1, n):
        peer = lax.rem(e + d, n)
        copy = remote(outgoing.at[peer], mine.at[e], s1.at[d], r1.at[d], (peer, c))
        copy.start()
        sends.append(copy)
    forwards = [remote(outgoing.at[e], theirs.at[e], fs.at[0], fr.at[0], (e, other))]
    forwards[0].start()
    mine[pl.ds(e, 1)] = outgoing[pl.ds(e, 1)]
    for d in range(1, n):
        sends[d - 1].wait_recv()
        source = lax.rem(e - d + n, n)
        copy = remote(mine.at[source], theirs.at[source], fs.at[d], fr.at[d], (e, other))
        copy.start()
        forwards.append(copy)

    def flat(ref):
        return ref[...].astype(F32).reshape(total, half).astype(BF16)

    for load in loads:
        load.wait()
    own_rows = flat(mine)
    gate = jnp.dot(own_rows, eg[own_cols, :], preferred_element_type=F32)
    up = jnp.dot(own_rows, eu[own_cols, :], preferred_element_type=F32)
    for copy in forwards:
        copy.wait_recv()
    other_rows = flat(theirs)
    gate = gate + jnp.dot(other_rows, eg[other_cols, :], preferred_element_type=F32)
    up = up + jnp.dot(other_rows, eu[other_cols, :], preferred_element_type=F32)
    hidden = (silu(gate) * up).astype(BF16)

    pieces = ds_.shape[0]
    span = n // pieces
    height = span * slots
    downs = []
    for piece in range(pieces):
        block = jnp.dot(
            hidden[piece * height : (piece + 1) * height], ed[:, other_cols],
            preferred_element_type=F32,
        )
        for at in range(span):
            down_out[piece * span + at] = block[at * slots : (at + 1) * slots].astype(BF16)
        here = pl.ds(piece * span, span)
        copy = remote(
            down_out.at[here], down_in.at[here], ds_.at[piece], dr.at[piece], (e, other)
        )
        copy.start()
        downs.append(copy)
    kept = jnp.dot(hidden, ed[:, own_cols], preferred_element_type=F32)
    for piece in range(pieces):
        downs[piece].wait_recv()
        for at in range(piece * span, (piece + 1) * span):
            own = kept[at * slots : (at + 1) * slots].astype(BF16).astype(F32)
            results[at] = (own + down_in[at].astype(F32)).astype(BF16)
    returns = []
    for d in range(1, n):
        peer = lax.rem(e + d, n)
        copy = remote(results.at[peer], back.at[e], s2.at[d], r2.at[d], (peer, c))
        copy.start()
        returns.append(copy)
    back[pl.ds(e, 1)] = results[pl.ds(e, 1)]
    for copy in returns:
        copy.wait_recv()
    picked = flat(back)
    moe_sum = jnp.dot(weigh_high, picked, preferred_element_type=F32) + jnp.dot(
        weigh_low, picked, preferred_element_type=F32
    )
    final = am_half.astype(F32) + moe_sum
    mean_own = jnp.mean(final, -1, keepdims=True)
    off = final - mean_own
    spread_own = jnp.sum(off * off, -1, keepdims=True)
    stat_lane = lax.broadcasted_iota(jnp.int32, stat_out.shape, 1)
    stat_out[...] = jnp.where(stat_lane < stat_out.shape[1] // 2, mean_own, spread_own)
    stats = remote(stat_out, stat_in, pair_sems.at[2], pair_sems.at[3], (e, other))
    stats.start()
    for copy in sends + forwards + downs + returns:
        copy.wait_send()
    stats.wait()
    mean_other = stat_in[:, 0:1]
    last = stat_in.shape[1]
    spread_other = stat_in[:, last - 1 : last]
    gap = mean_other - mean_own
    variance = (spread_own + spread_other + gap * gap * (half / 2)) / width
    gain = moe_gain[:, own_cols]
    out[...] = ((off - 0.5 * gap) * lax.rsqrt(variance + 1e-05) * gain).astype(BF16)


def per_device(
    tokens, old_state, w_query, w_forget, w_value, w_gate, lower_bound, head_gain, w_out,
    mix_gain, expert_gate, expert_up, expert_down, expert_ids, route_weight, moe_gain,
):
    rows, width = tokens.shape
    heads, state_width = old_state.shape[1:]
    hd = head_gain.shape[0]
    cols = w_query.shape[1]
    n = lax.axis_size("ep")
    half = width // lax.axis_size("tp")
    top = expert_ids.shape[1]
    capacity = max(2, 2 * top * rows // n)
    slots = -(-capacity // 8) * 8
    vmem = pl.BlockSpec(memory_space=pltpu.VMEM)
    hbm = pl.BlockSpec(memory_space=pl.ANY)
    new_state, part = pl.pallas_call(
        mixer_kernel,
        out_shape=(
            jax.ShapeDtypeStruct(old_state.shape, F32),
            jax.ShapeDtypeStruct((rows, width), BF16),
        ),
        in_specs=[vmem] * 3 + [hbm] * 6,
        out_specs=(hbm, vmem),
        scratch_shapes=[
            pltpu.VMEM((width, cols), BF16),
            pltpu.VMEM((width, cols), BF16),
            pltpu.VMEM((width, cols), BF16),
            pltpu.VMEM((width, cols), BF16),
            pltpu.VMEM((cols, width), BF16),
            pltpu.VMEM(old_state.shape, F32),
            pltpu.VMEM(old_state.shape, F32),
            pltpu.VMEM((2 * hd, state_width), BF16),
            pltpu.VMEM((rows, heads, 2 * hd), F32),
            pltpu.VMEM((rows, heads, 2 * hd), F32),
            pltpu.VMEM((rows, heads, 2 * hd), F32),
            pltpu.VMEM((rows, heads, hd), F32),
            pltpu.VMEM((rows, cols), F32),
            pltpu.SemaphoreType.DMA((6,)),
            pltpu.SemaphoreType.DMA((4,)),
        ],
        compiler_params=pltpu.CompilerParams(vmem_limit_bytes=48 * 1024 * 1024),
        name="mixer",
    )(
        tokens, lower_bound.reshape(1, cols), head_gain.reshape(1, hd),
        old_state, w_query, w_forget, w_value, w_gate, w_out,
    )
    ff = expert_gate.shape[2]
    slab = pltpu.VMEM((n, slots, half), BF16)
    pieces = 4
    dma = pltpu.SemaphoreType.DMA
    next_tokens = pl.pallas_call(
        functools.partial(expert_kernel, capacity, n),
        out_shape=jax.ShapeDtypeStruct((rows, half), BF16),
        in_specs=[vmem] * 6 + [hbm] * 3,
        out_specs=vmem,
        scratch_shapes=[
            pltpu.VMEM((width, ff), BF16),
            pltpu.VMEM((width, ff), BF16),
            pltpu.VMEM((ff, width), BF16),
            pltpu.VMEM((rows, width), BF16),
            pltpu.VMEM((rows, width), F32),
            slab, slab, slab, slab, slab, slab, slab,
            pltpu.VMEM((rows, 128), F32),
            pltpu.VMEM((rows, 128), F32),
            dma((3,)), dma((4,)), dma((n,)), dma((n,)), dma((n,)), dma((n,)), dma((n,)), dma((n,)),
            dma((pieces,)), dma((pieces,)),
        ],
        compiler_params=pltpu.CompilerParams(
            collective_id=0, has_side_effects=True, vmem_limit_bytes=48 * 1024 * 1024
        ),
        name="experts",
    )(
        part, tokens, mix_gain.reshape(1, width), expert_ids, route_weight,
        moe_gain.reshape(1, width), expert_gate.reshape(width, ff), expert_up.reshape(width, ff),
        expert_down.reshape(ff, width),
    )
    return (next_tokens, new_state)


def solution(mesh):
    in_specs = (
        P("ep", None),
        P("ep", "tp", None),
        P(None, "tp"),
        P(None, "tp"),
        P(None, "tp"),
        P(None, "tp"),
        P("tp"),
        P(),
        P("tp", None),
        P(),
        P("ep", None, "tp"),
        P("ep", None, "tp"),
        P("ep", "tp", None),
        P("ep", None),
        P("ep", None),
        P(),
    )
    out_specs = (P("ep", "tp"), P("ep", "tp", None))
    return jax.shard_map(
        per_device, mesh=mesh, in_specs=in_specs, out_specs=out_specs, check_vma=False
    )
```

```python
import functools

import jax
import jax.numpy as jnp
from jax import lax
from jax.experimental import pallas as pl
from jax.experimental.pallas import tpu as pltpu
from jax.sharding import PartitionSpec as P

F32 = jnp.float32
BF16 = jnp.bfloat16
MESH = pl.DeviceIdType.MESH
GRANT = 67043328 - 512 * 1024


def silu(values):
    return values * jax.nn.sigmoid(values)


def mixer_kernel(
    tok_hbm, lb_hbm, hg_hbm, st_hbm, wq_hbm, wf_hbm, wv_hbm, wg_hbm, wo_hbm,
    ns_hbm, part,
    tok, lb, hg, wq, wf, wv, wg, wo, st, ns, spread, qs, fs, vs, ro, mix, sems, out_sems,
):
    rows, heads, width = st.shape
    hd = hg.shape[1]
    loads = [
        pltpu.make_async_copy(src, dst, sems.at[at])
        for at, (src, dst) in enumerate(
            ((wf_hbm, wf), (wv_hbm, wv), (wq_hbm, wq), (st_hbm, st), (wg_hbm, wg), (wo_hbm, wo))
        )
    ]
    smalls = [
        pltpu.make_async_copy(src, dst, sems.at[len(loads) + at])
        for at, (src, dst) in enumerate(((tok_hbm, tok), (lb_hbm, lb), (hg_hbm, hg)))
    ]
    for load in smalls + loads:
        load.start()
    key_of = lax.broadcasted_iota(jnp.int32, spread.shape, 0) % hd
    lane_key = lax.broadcasted_iota(jnp.int32, spread.shape, 1) // hd
    spread[...] = jnp.where(key_of == lane_key, 1.0, 0.0).astype(BF16)

    def split_heads(values, ref):
        high = values.astype(BF16).astype(F32)
        low = values - high
        for h in range(heads):
            at = slice(h * hd, (h + 1) * hd)
            ref[:, h, 0:hd] = high[:, at]
            ref[:, h, hd : 2 * hd] = low[:, at]

    for load in smalls:
        load.wait()
    tokens = tok[...]
    loads[0].wait()
    f_lin = jnp.dot(tokens, wf[...], preferred_element_type=F32)
    bound = lb[...]
    split_heads(bound + (1.0 - bound) * jax.nn.sigmoid(f_lin), fs)
    loads[1].wait()
    v_lin = jnp.dot(tokens, wv[...], preferred_element_type=F32)
    for h in range(heads):
        at = slice(h * hd, (h + 1) * hd)
        vs[:, h, 0:hd] = v_lin[:, at]
        vs[:, h, hd : 2 * hd] = v_lin[:, at]
    loads[2].wait()
    q_lin = jnp.dot(tokens, wq[...], preferred_element_type=F32)
    split_heads(silu(q_lin), qs)
    loads[3].wait()
    flat = (rows * heads, 2 * hd)
    keep = fs[...].reshape(flat).astype(BF16)
    ask = qs[...].reshape(flat).astype(BF16)
    value = vs[...]
    pair = 2 * hd
    block = 2 * pair
    chunks = out_sems.shape[0]
    per_chunk = width // chunks
    acc = jnp.zeros((rows, heads, pair), F32)
    stores = []
    for chunk in range(chunks):

        def step(i, acc, chunk=chunk):
            start = pl.multiple_of(chunk * per_chunk + i * block, block)
            ones = spread[:, pl.ds(start, block)]
            f_wide = jnp.dot(keep, ones, preferred_element_type=F32).reshape(rows, heads, block)
            q_wide = jnp.dot(ask, ones, preferred_element_type=F32).reshape(rows, heads, block)
            for half in range(2):
                lanes = pl.ds(pl.multiple_of(start + half * pair, pair), pair)
                cut = slice(half * pair, (half + 1) * pair)
                new = value + f_wide[:, :, cut] * (st[:, :, lanes] - value)
                ns[:, :, lanes] = new
                acc = acc + q_wide[:, :, cut] * new
            return acc

        acc = lax.fori_loop(0, per_chunk // block, step, acc)
        span = pl.ds(chunk * per_chunk, per_chunk)
        store = pltpu.make_async_copy(ns.at[:, :, span], ns_hbm.at[:, :, span], out_sems.at[chunk])
        store.start()
        stores.append(store)
    readout = acc[:, :, 0:hd] + acc[:, :, hd:pair]
    square = jnp.mean(readout * readout, -1, keepdims=True)
    ro[...] = readout * lax.rsqrt(square + 1e-06) * hg[...].reshape(1, 1, hd)
    for h in range(heads):
        mix[:, h * hd : (h + 1) * hd] = ro[:, h, :]
    loads[4].wait()
    g_lin = jnp.dot(tokens, wg[...], preferred_element_type=F32)
    mixer_out = (mix[...] * silu(g_lin)).astype(BF16)
    loads[5].wait()
    part[...] = jnp.dot(mixer_out, wo[...], preferred_element_type=F32).astype(BF16)
    for store in stores:
        store.wait()


def expert_kernel(
    capacity, n,
    part_hbm, tok_hbm, mix_hbm, ids_hbm, route_hbm, moe_hbm, eg_hbm, eu_hbm, ed_hbm,
    out,
    part, tok, mix_gain, ids, route, moe_gain,
    eg, eu, ed, part_in, am, outgoing, mine, theirs, down_out, down_in, results, back,
    stat_out, stat_in,
    w_sems, pair_sems, s1, r1, s2, r2, fs, fr, ds_, dr,
):
    e = lax.axis_index("ep")
    c = lax.axis_index("tp")
    other = 1 - c
    rows, width = tok.shape
    slots, wide = outgoing.shape[1:]
    half = width // 2
    quarter = half - wide
    folds = wide // quarter if quarter else 0
    total = n * slots
    barrier = pltpu.get_barrier_semaphore()
    pl.semaphore_signal(barrier, inc=1, device_id=(e, other), device_id_type=MESH)
    for d in range(1, n):
        pl.semaphore_signal(barrier, inc=1, device_id=(lax.rem(e + d, n), c), device_id_type=MESH)
    loads = [
        pltpu.make_async_copy(src, dst, w_sems.at[at])
        for at, (src, dst) in enumerate(
            (
                (ids_hbm, ids), (route_hbm, route), (part_hbm, part), (tok_hbm, tok),
                (mix_hbm, mix_gain), (moe_hbm, moe_gain),
                (eg_hbm, eg), (eu_hbm, eu), (ed_hbm, ed),
            )
        )
    ]
    for load in loads:
        load.start()

    def remote(src, dst, send, recv, device):
        return pltpu.make_async_remote_copy(
            src_ref=src, dst_ref=dst, send_sem=send, recv_sem=recv,
            device_id=device, device_id_type=MESH,
        )

    for load in loads[:6]:
        load.wait()
    slot = lax.broadcasted_iota(jnp.int32, (total, rows), 0)
    slot_expert = slot // slots
    slot_rank = slot % slots
    first = jnp.where(ids[0:1, :] == slot_expert, 1.0, 0.0)
    second = jnp.where(ids[1:2, :] == slot_expert, 1.0, 0.0)
    named = first + second
    row_at = lax.broadcasted_iota(jnp.int32, (rows, rows), 0)
    col_at = lax.broadcasted_iota(jnp.int32, (rows, rows), 1)
    earlier = jnp.where(row_at < col_at, 1.0, 0.0).astype(BF16)
    before = jnp.dot(named.astype(BF16), earlier, preferred_element_type=F32)
    places = [jnp.where(before == slot_rank.astype(F32), named, 0.0)]
    for p in range(folds):
        rank = (slot_rank - capacity) * folds + p
        hit = (before == rank.astype(F32)) & (slot_rank >= capacity)
        places.append(jnp.where(hit, named, 0.0))
    route_of = first * route[0:1, :] + second * route[1:2, :]
    weighs = []
    for place in places:
        weigh = jnp.transpose(place * route_of)
        high = weigh.astype(BF16).astype(F32)
        weighs.append(jnp.concatenate([high, weigh - high], 0).astype(BF16))
    places = [place.astype(BF16) for place in places]
    to_at = lax.broadcasted_iota(jnp.int32, (total, total), 0)
    from_at = lax.broadcasted_iota(jnp.int32, (total, total), 1)
    together = to_at // slots == from_at // slots
    unfold, refold = [], []
    for p in range(folds):
        to_rank, from_rank = to_at % slots, from_at % slots
        un = together & (from_rank >= capacity) & (to_rank == (from_rank - capacity) * folds + p)
        re = together & (to_rank >= capacity) & (from_rank == (to_rank - capacity) * folds + p)
        unfold.append(jnp.where(un, 1.0, 0.0).astype(BF16))
        refold.append(jnp.where(re, 1.0, 0.0).astype(BF16))

    def cut(values, p):
        return values[:, p * quarter : (p + 1) * quarter]

    pl.semaphore_wait(barrier, n)
    swap = remote(part_hbm, part_in, pair_sems.at[0], pair_sems.at[1], (e, other))
    swap.start()
    base = tok[...].astype(F32) + part[...].astype(F32)
    swap.wait()
    values = base + part_in[...].astype(F32)
    centered = values - jnp.mean(values, -1, keepdims=True)
    variance = jnp.mean(centered * centered, -1, keepdims=True)
    am[...] = centered * lax.rsqrt(variance + 1e-05) * mix_gain[...]

    own_cols = pl.ds(pl.multiple_of(c * half, half), half)
    other_cols = pl.ds(pl.multiple_of(other * half, half), half)
    am_half = am[:, own_cols].astype(BF16)
    sent = jnp.dot(places[0], am_half[:, 0:wide], preferred_element_type=F32)
    if folds:
        tail = am_half[:, wide:half]
        sent = sent + jnp.concatenate(
            [jnp.dot(place, tail, preferred_element_type=F32) for place in places[1:]], 1
        )
    for at in range(n):
        outgoing[at] = sent[at * slots : (at + 1) * slots].astype(BF16)
    sends = []
    for d in range(1, n):
        peer = lax.rem(e + d, n)
        copy = remote(outgoing.at[peer], mine.at[e], s1.at[d], r1.at[d], (peer, c))
        copy.start()
        sends.append(copy)
    forwards = [remote(outgoing.at[e], theirs.at[e], fs.at[0], fr.at[0], (e, other))]
    forwards[0].start()
    mine[pl.ds(e, 1)] = outgoing[pl.ds(e, 1)]
    for d in range(1, n):
        sends[d - 1].wait_recv()
        source = lax.rem(e - d + n, n)
        copy = remote(mine.at[source], theirs.at[source], fs.at[d], fr.at[d], (e, other))
        copy.start()
        forwards.append(copy)

    def flat(ref):
        return ref[...].astype(F32).reshape(total, wide).astype(BF16)

    def gate_and_up(ref, side):
        block = flat(ref)
        start = pl.multiple_of(side * half, half)
        cols = pl.ds(start, wide)
        gate = jnp.dot(block, eg[cols, :], preferred_element_type=F32)
        up = jnp.dot(block, eu[cols, :], preferred_element_type=F32)
        if folds:
            tail = jnp.zeros((total, quarter), F32)
            for p in range(folds):
                tail = tail + jnp.dot(unfold[p], cut(block, p), preferred_element_type=F32)
            tail = tail.astype(BF16)
            cols = pl.ds(pl.multiple_of(start + wide, quarter), quarter)
            gate = gate + jnp.dot(tail, eg[cols, :], preferred_element_type=F32)
            up = up + jnp.dot(tail, eu[cols, :], preferred_element_type=F32)
        return gate, up

    for load in loads[6:]:
        load.wait()
    gate, up = gate_and_up(mine, c)
    for copy in forwards:
        copy.wait_recv()
    gate_more, up_more = gate_and_up(theirs, other)
    hidden = silu(gate + gate_more) * (up + up_more)
    hidden_rank = lax.broadcasted_iota(jnp.int32, hidden.shape, 0) % slots
    hidden = jnp.where(hidden_rank < capacity, hidden, 0.0).astype(BF16)

    pieces = ds_.shape[0]
    span = n // pieces
    height = span * slots

    def down(piece, cols):
        block = jnp.dot(
            hidden[piece * height : (piece + 1) * height], ed[:, cols],
            preferred_element_type=F32,
        ).astype(BF16)
        if folds:
            tail = block[:, wide:half]
            block = block[:, 0:wide].astype(F32) + jnp.concatenate(
                [
                    jnp.dot(one[0:height, 0:height], tail, preferred_element_type=F32)
                    for one in refold
                ],
                1,
            )
        return block.astype(F32)

    downs = []
    for piece in range(pieces):
        block = down(piece, other_cols)
        for at in range(span):
            down_out[piece * span + at] = block[at * slots : (at + 1) * slots].astype(BF16)
        here = pl.ds(piece * span, span)
        copy = remote(
            down_out.at[here], down_in.at[here], ds_.at[piece], dr.at[piece], (e, other)
        )
        copy.start()
        downs.append(copy)
    kept = [down(piece, own_cols) for piece in range(pieces)]
    for piece in range(pieces):
        downs[piece].wait_recv()
        for at in range(span):
            own = kept[piece][at * slots : (at + 1) * slots]
            results[piece * span + at] = (own + down_in[piece * span + at].astype(F32)).astype(BF16)
    returns = []
    for d in range(1, n):
        peer = lax.rem(e + d, n)
        copy = remote(results.at[peer], back.at[e], s2.at[d], r2.at[d], (peer, c))
        copy.start()
        returns.append(copy)
    back[pl.ds(e, 1)] = results[pl.ds(e, 1)]
    for copy in returns:
        copy.wait_recv()
    picked = flat(back)

    def weighted(weigh, block):
        both = jnp.dot(weigh, block, preferred_element_type=F32)
        return both[0:rows] + both[rows : 2 * rows]

    moe_sum = weighted(weighs[0], picked)
    if folds:
        tail = jnp.zeros((rows, quarter), F32)
        for p in range(folds):
            tail = tail + weighted(weighs[1 + p], cut(picked, p))
        moe_sum = jnp.concatenate([moe_sum, tail], 1)
    final = am_half.astype(F32) + moe_sum
    mean_own = jnp.mean(final, -1, keepdims=True)
    off = final - mean_own
    spread_own = jnp.sum(off * off, -1, keepdims=True)
    stat_lane = lax.broadcasted_iota(jnp.int32, stat_out.shape, 1)
    stat_out[...] = jnp.where(stat_lane < stat_out.shape[1] // 2, mean_own, spread_own)
    stats = remote(stat_out, stat_in, pair_sems.at[2], pair_sems.at[3], (e, other))
    stats.start()
    for copy in sends + forwards + downs + returns:
        copy.wait_send()
    stats.wait()
    mean_other = stat_in[:, 0:1]
    last = stat_in.shape[1]
    spread_other = stat_in[:, last - 1 : last]
    gap = mean_other - mean_own
    variance = (spread_own + spread_other + gap * gap * (half / 2)) / width
    gain = moe_gain[:, own_cols]
    out[...] = ((off - 0.5 * gap) * lax.rsqrt(variance + 1e-05) * gain).astype(BF16)


def per_device(
    tokens, old_state, w_query, w_forget, w_value, w_gate, lower_bound, head_gain, w_out,
    mix_gain, expert_gate, expert_up, expert_down, expert_ids, route_weight, moe_gain,
):
    rows, width = tokens.shape
    heads, state_width = old_state.shape[1:]
    hd = head_gain.shape[0]
    cols = w_query.shape[1]
    n = lax.axis_size("ep")
    half = width // lax.axis_size("tp")
    top = expert_ids.shape[1]
    capacity = max(2, 2 * top * rows // n)
    slots = -(-capacity // 8) * 8
    vmem = pl.BlockSpec(memory_space=pltpu.VMEM)
    hbm = pl.BlockSpec(memory_space=pltpu.MemorySpace.HBM)
    new_state, part = pl.pallas_call(
        mixer_kernel,
        out_shape=(
            jax.ShapeDtypeStruct(old_state.shape, F32),
            jax.ShapeDtypeStruct((rows, width), BF16),
        ),
        in_specs=[hbm] * 9,
        out_specs=(hbm, vmem),
        scratch_shapes=[
            pltpu.VMEM((rows, width), BF16),
            pltpu.VMEM((1, cols), F32),
            pltpu.VMEM((1, hd), F32),
            pltpu.VMEM((width, cols), BF16),
            pltpu.VMEM((width, cols), BF16),
            pltpu.VMEM((width, cols), BF16),
            pltpu.VMEM((width, cols), BF16),
            pltpu.VMEM((cols, width), BF16),
            pltpu.VMEM(old_state.shape, F32),
            pltpu.VMEM(old_state.shape, F32),
            pltpu.VMEM((2 * hd, state_width), BF16),
            pltpu.VMEM((rows, heads, 2 * hd), F32),
            pltpu.VMEM((rows, heads, 2 * hd), F32),
            pltpu.VMEM((rows, heads, 2 * hd), F32),
            pltpu.VMEM((rows, heads, hd), F32),
            pltpu.VMEM((rows, cols), F32),
            pltpu.SemaphoreType.DMA((9,)),
            pltpu.SemaphoreType.DMA((4,)),
        ],
        compiler_params=pltpu.CompilerParams(vmem_limit_bytes=GRANT),
        name="mixer",
    )(
        tokens, lower_bound.reshape(1, cols), head_gain.reshape(1, hd),
        old_state, w_query, w_forget, w_value, w_gate, w_out,
    )
    ff = expert_gate.shape[2]
    spare = slots - capacity
    wide = half
    if spare and capacity % spare == 0 and half % ((capacity // spare + 1) * 128) == 0:
        wide = half // (capacity // spare + 1) * (capacity // spare)
    slab = pltpu.VMEM((n, slots, wide), BF16)
    pieces = 4
    dma = pltpu.SemaphoreType.DMA
    next_tokens = pl.pallas_call(
        functools.partial(expert_kernel, capacity, n),
        out_shape=jax.ShapeDtypeStruct((rows, half), BF16),
        in_specs=[hbm] * 9,
        out_specs=vmem,
        scratch_shapes=[
            pltpu.VMEM((rows, width), BF16),
            pltpu.VMEM((rows, width), BF16),
            pltpu.VMEM((1, width), F32),
            pltpu.VMEM((top, rows), jnp.int32),
            pltpu.VMEM((top, rows), F32),
            pltpu.VMEM((1, width), F32),
            pltpu.VMEM((width, ff), BF16),
            pltpu.VMEM((width, ff), BF16),
            pltpu.VMEM((ff, width), BF16),
            pltpu.VMEM((rows, width), BF16),
            pltpu.VMEM((rows, width), F32),
            slab, slab, slab, slab, slab, slab, slab,
            pltpu.VMEM((rows, 128), F32),
            pltpu.VMEM((rows, 128), F32),
            dma((9,)), dma((4,)), dma((n,)), dma((n,)), dma((n,)), dma((n,)), dma((n,)), dma((n,)),
            dma((pieces,)), dma((pieces,)),
        ],
        compiler_params=pltpu.CompilerParams(
            collective_id=0, has_side_effects=True, vmem_limit_bytes=GRANT
        ),
        name="experts",
    )(
        part, tokens, mix_gain.reshape(1, width), expert_ids.T, route_weight.T,
        moe_gain.reshape(1, width), expert_gate.reshape(width, ff), expert_up.reshape(width, ff),
        expert_down.reshape(ff, width),
    )
    return (next_tokens, new_state)


def solution(mesh):
    in_specs = (
        P("ep", None),
        P("ep", "tp", None),
        P(None, "tp"),
        P(None, "tp"),
        P(None, "tp"),
        P(None, "tp"),
        P("tp"),
        P(),
        P("tp", None),
        P(),
        P("ep", None, "tp"),
        P("ep", None, "tp"),
        P("ep", "tp", None),
        P("ep", None),
        P("ep", None),
        P(),
    )
    out_specs = (P("ep", "tp"), P("ep", "tp", None))
    return jax.shard_map(
        per_device, mesh=mesh, in_specs=in_specs, out_specs=out_specs, check_vma=False
    )
```

```python
import functools

import jax
import jax.numpy as jnp
from jax import lax
from jax.experimental import pallas as pl
from jax.experimental.pallas import tpu as pltpu
from jax.sharding import PartitionSpec as P

F32 = jnp.float32
BF16 = jnp.bfloat16
MESH = pl.DeviceIdType.MESH
GRANT = 67043328 - 512 * 1024


def silu(values):
    return values * jax.nn.sigmoid(values)


def mixer_kernel(
    tok_hbm, lb_hbm, hg_hbm, st_hbm, wq_hbm, wf_hbm, wv_hbm, wg_hbm, wo_hbm,
    ns_hbm, part,
    tok, lb, hg, wq, wf, wv, wg, wo, st, ns, spread, qs, fs, vs, ro, mix, sems, out_sems,
):
    rows, heads, width = st.shape
    hd = hg.shape[1]
    loads = [
        pltpu.make_async_copy(src, dst, sems.at[at])
        for at, (src, dst) in enumerate(
            ((wf_hbm, wf), (wv_hbm, wv), (wq_hbm, wq), (st_hbm, st), (wg_hbm, wg), (wo_hbm, wo))
        )
    ]
    smalls = [
        pltpu.make_async_copy(src, dst, sems.at[len(loads) + at])
        for at, (src, dst) in enumerate(((tok_hbm, tok), (lb_hbm, lb), (hg_hbm, hg)))
    ]
    for load in smalls + loads:
        load.start()
    key_of = lax.broadcasted_iota(jnp.int32, spread.shape, 0) % hd
    lane_key = lax.broadcasted_iota(jnp.int32, spread.shape, 1) // hd
    spread[...] = jnp.where(key_of == lane_key, 1.0, 0.0).astype(BF16)

    def split_heads(values, ref):
        high = values.astype(BF16).astype(F32)
        low = values - high
        for h in range(heads):
            at = slice(h * hd, (h + 1) * hd)
            ref[:, h, 0:hd] = high[:, at]
            ref[:, h, hd : 2 * hd] = low[:, at]

    for load in smalls:
        load.wait()
    tokens = tok[...]
    loads[0].wait()
    f_lin = jnp.dot(tokens, wf[...], preferred_element_type=F32)
    bound = lb[...]
    split_heads(bound + (1.0 - bound) * jax.nn.sigmoid(f_lin), fs)
    loads[1].wait()
    v_lin = jnp.dot(tokens, wv[...], preferred_element_type=F32)
    for h in range(heads):
        at = slice(h * hd, (h + 1) * hd)
        vs[:, h, 0:hd] = v_lin[:, at]
        vs[:, h, hd : 2 * hd] = v_lin[:, at]
    loads[2].wait()
    q_lin = jnp.dot(tokens, wq[...], preferred_element_type=F32)
    split_heads(silu(q_lin), qs)
    loads[3].wait()
    flat = (rows * heads, 2 * hd)
    keep = fs[...].reshape(flat).astype(BF16)
    ask = qs[...].reshape(flat).astype(BF16)
    value = vs[...]
    pair = 2 * hd
    block = 2 * pair
    chunks = out_sems.shape[0]
    per_chunk = width // chunks
    acc = jnp.zeros((rows, heads, pair), F32)
    stores = []
    for chunk in range(chunks):

        def step(i, acc, chunk=chunk):
            start = pl.multiple_of(chunk * per_chunk + i * block, block)
            ones = spread[:, pl.ds(start, block)]
            f_wide = jnp.dot(keep, ones, preferred_element_type=F32).reshape(rows, heads, block)
            q_wide = jnp.dot(ask, ones, preferred_element_type=F32).reshape(rows, heads, block)
            for half in range(2):
                lanes = pl.ds(pl.multiple_of(start + half * pair, pair), pair)
                cut = slice(half * pair, (half + 1) * pair)
                new = value + f_wide[:, :, cut] * (st[:, :, lanes] - value)
                ns[:, :, lanes] = new
                acc = acc + q_wide[:, :, cut] * new
            return acc

        acc = lax.fori_loop(0, per_chunk // block, step, acc)
        span = pl.ds(chunk * per_chunk, per_chunk)
        store = pltpu.make_async_copy(ns.at[:, :, span], ns_hbm.at[:, :, span], out_sems.at[chunk])
        store.start()
        stores.append(store)
    readout = acc[:, :, 0:hd] + acc[:, :, hd:pair]
    square = jnp.mean(readout * readout, -1, keepdims=True)
    ro[...] = readout * lax.rsqrt(square + 1e-06) * hg[...].reshape(1, 1, hd)
    for h in range(heads):
        mix[:, h * hd : (h + 1) * hd] = ro[:, h, :]
    loads[4].wait()
    g_lin = jnp.dot(tokens, wg[...], preferred_element_type=F32)
    mixer_out = (mix[...] * silu(g_lin)).astype(BF16)
    loads[5].wait()
    part[...] = jnp.dot(mixer_out, wo[...], preferred_element_type=F32).astype(BF16)
    for store in stores:
        store.wait()


def expert_kernel(
    capacity, n,
    part_hbm, tok_hbm, mix_hbm, ids_hbm, route_hbm, moe_hbm, eg_hbm, eu_hbm, ed_hbm,
    out,
    part, tok, mix_gain, ids, route, moe_gain,
    eg, eu, ed, part_in, am, outgoing, mine, theirs, down_out, down_in, results, back,
    stat_out, stat_in,
    w_sems, pair_sems, s1, r1, s2, r2, fs, fr, ds_, dr,
):
    e = lax.axis_index("ep")
    c = lax.axis_index("tp")
    other = 1 - c
    rows, width = tok.shape
    slots, wide = outgoing.shape[1:]
    half = width // 2
    quarter = half - wide
    folds = wide // quarter if quarter else 0
    total = n * slots
    barrier = pltpu.get_barrier_semaphore()
    pl.semaphore_signal(barrier, inc=1, device_id=(e, other), device_id_type=MESH)
    for d in range(1, n):
        pl.semaphore_signal(barrier, inc=1, device_id=(lax.rem(e + d, n), c), device_id_type=MESH)
    loads = [
        pltpu.make_async_copy(src, dst, w_sems.at[at])
        for at, (src, dst) in enumerate(
            (
                (ids_hbm, ids), (route_hbm, route), (part_hbm, part), (tok_hbm, tok),
                (mix_hbm, mix_gain), (moe_hbm, moe_gain),
                (eg_hbm, eg), (eu_hbm, eu), (ed_hbm, ed),
            )
        )
    ]
    for load in loads:
        load.start()

    def remote(src, dst, send, recv, device):
        return pltpu.make_async_remote_copy(
            src_ref=src, dst_ref=dst, send_sem=send, recv_sem=recv,
            device_id=device, device_id_type=MESH,
        )

    for load in loads[:6]:
        load.wait()
    slot = lax.broadcasted_iota(jnp.int32, (total, rows), 0)
    slot_expert = slot // slots
    slot_rank = slot % slots
    first = jnp.where(ids[0:1, :] == slot_expert, 1.0, 0.0)
    second = jnp.where(ids[1:2, :] == slot_expert, 1.0, 0.0)
    named = first + second
    row_at = lax.broadcasted_iota(jnp.int32, (rows, rows), 0)
    col_at = lax.broadcasted_iota(jnp.int32, (rows, rows), 1)
    earlier = jnp.where(row_at < col_at, 1.0, 0.0).astype(BF16)
    before = jnp.dot(named.astype(BF16), earlier, preferred_element_type=F32)
    places = [jnp.where(before == slot_rank.astype(F32), named, 0.0)]
    for p in range(folds):
        rank = (slot_rank - capacity) * folds + p
        hit = (before == rank.astype(F32)) & (slot_rank >= capacity)
        places.append(jnp.where(hit, named, 0.0))
    route_of = first * route[0:1, :] + second * route[1:2, :]
    weighs = []
    for place in places:
        weigh = jnp.transpose(place * route_of)
        high = weigh.astype(BF16).astype(F32)
        weighs.append(jnp.concatenate([high, weigh - high], 0).astype(BF16))
    places = [place.astype(BF16) for place in places]
    to_at = lax.broadcasted_iota(jnp.int32, (total, total), 0)
    from_at = lax.broadcasted_iota(jnp.int32, (total, total), 1)
    together = to_at // slots == from_at // slots
    unfold, refold = [], []
    for p in range(folds):
        to_rank, from_rank = to_at % slots, from_at % slots
        un = together & (from_rank >= capacity) & (to_rank == (from_rank - capacity) * folds + p)
        re = together & (to_rank >= capacity) & (from_rank == (to_rank - capacity) * folds + p)
        unfold.append(jnp.where(un, 1.0, 0.0).astype(BF16))
        refold.append(jnp.where(re, 1.0, 0.0).astype(BF16))

    def cut(values, p):
        return values[:, p * quarter : (p + 1) * quarter]

    pl.semaphore_wait(barrier, n)
    swap = remote(part_hbm, part_in, pair_sems.at[0], pair_sems.at[1], (e, other))
    swap.start()
    base = tok[...].astype(F32) + part[...].astype(F32)
    swap.wait()
    values = base + part_in[...].astype(F32)
    centered = values - jnp.mean(values, -1, keepdims=True)
    variance = jnp.mean(centered * centered, -1, keepdims=True)
    am[...] = centered * lax.rsqrt(variance + 1e-05) * mix_gain[...]

    own_cols = pl.ds(pl.multiple_of(c * half, half), half)
    other_cols = pl.ds(pl.multiple_of(other * half, half), half)
    am_half = am[:, own_cols].astype(BF16)
    sent = jnp.dot(places[0], am_half[:, 0:wide], preferred_element_type=F32)
    if folds:
        tail = am_half[:, wide:half]
        sent = sent + jnp.concatenate(
            [jnp.dot(place, tail, preferred_element_type=F32) for place in places[1:]], 1
        )
    for at in range(n):
        outgoing[at] = sent[at * slots : (at + 1) * slots].astype(BF16)
    sends = []
    for d in range(1, n):
        peer = lax.rem(e + d, n)
        copy = remote(outgoing.at[peer], mine.at[e], s1.at[d], r1.at[d], (peer, c))
        copy.start()
        sends.append(copy)
    forwards = [remote(outgoing.at[e], theirs.at[e], fs.at[0], fr.at[0], (e, other))]
    forwards[0].start()
    mine[pl.ds(e, 1)] = outgoing[pl.ds(e, 1)]
    for d in range(1, n):
        sends[d - 1].wait_recv()
        source = lax.rem(e - d + n, n)
        copy = remote(mine.at[source], theirs.at[source], fs.at[d], fr.at[d], (e, other))
        copy.start()
        forwards.append(copy)

    def flat(ref):
        return ref[...].astype(F32).reshape(total, wide).astype(BF16)

    def gate_and_up(ref, side):
        block = flat(ref)
        start = pl.multiple_of(side * half, half)
        cols = pl.ds(start, wide)
        gate = jnp.dot(block, eg[cols, :], preferred_element_type=F32)
        up = jnp.dot(block, eu[cols, :], preferred_element_type=F32)
        if folds:
            tail = jnp.zeros((total, quarter), F32)
            for p in range(folds):
                tail = tail + jnp.dot(unfold[p], cut(block, p), preferred_element_type=F32)
            tail = tail.astype(BF16)
            cols = pl.ds(pl.multiple_of(start + wide, quarter), quarter)
            gate = gate + jnp.dot(tail, eg[cols, :], preferred_element_type=F32)
            up = up + jnp.dot(tail, eu[cols, :], preferred_element_type=F32)
        return gate, up

    for load in loads[6:]:
        load.wait()
    gate, up = gate_and_up(mine, c)
    for copy in forwards:
        copy.wait_recv()
    gate_more, up_more = gate_and_up(theirs, other)
    hidden = silu(gate + gate_more) * (up + up_more)
    hidden_rank = lax.broadcasted_iota(jnp.int32, hidden.shape, 0) % slots
    hidden = jnp.where(hidden_rank < capacity, hidden, 0.0).astype(BF16)

    pieces = ds_.shape[0]
    span = n // pieces
    height = span * slots

    def down(piece, cols):
        block = jnp.dot(
            hidden[piece * height : (piece + 1) * height], ed[:, cols],
            preferred_element_type=F32,
        ).astype(BF16)
        if folds:
            tail = block[:, wide:half]
            block = block[:, 0:wide].astype(F32) + jnp.concatenate(
                [
                    jnp.dot(one[0:height, 0:height], tail, preferred_element_type=F32)
                    for one in refold
                ],
                1,
            )
        return block.astype(F32)

    downs = []
    for piece in range(pieces):
        block = down(piece, other_cols)
        for at in range(span):
            down_out[piece * span + at] = block[at * slots : (at + 1) * slots].astype(BF16)
        here = pl.ds(piece * span, span)
        copy = remote(
            down_out.at[here], down_in.at[here], ds_.at[piece], dr.at[piece], (e, other)
        )
        copy.start()
        downs.append(copy)
    kept = [down(piece, own_cols) for piece in range(pieces)]
    for piece in range(pieces):
        downs[piece].wait_recv()
        for at in range(span):
            own = kept[piece][at * slots : (at + 1) * slots]
            results[piece * span + at] = (own + down_in[piece * span + at].astype(F32)).astype(BF16)
    returns = []
    for d in range(1, n):
        peer = lax.rem(e + d, n)
        copy = remote(results.at[peer], back.at[e], s2.at[d], r2.at[d], (peer, c))
        copy.start()
        returns.append(copy)
    back[pl.ds(e, 1)] = results[pl.ds(e, 1)]
    for copy in returns:
        copy.wait_recv()
    picked = flat(back)

    def weighted(weigh, block):
        both = jnp.dot(weigh, block, preferred_element_type=F32)
        return both[0:rows] + both[rows : 2 * rows]

    moe_sum = weighted(weighs[0], picked)
    if folds:
        tail = jnp.zeros((rows, quarter), F32)
        for p in range(folds):
            tail = tail + weighted(weighs[1 + p], cut(picked, p))
        moe_sum = jnp.concatenate([moe_sum, tail], 1)
    final = am_half.astype(F32) + moe_sum
    mean_own = jnp.mean(final, -1, keepdims=True)
    off = final - mean_own
    spread_own = jnp.sum(off * off, -1, keepdims=True)
    stat_lane = lax.broadcasted_iota(jnp.int32, stat_out.shape, 1)
    stat_out[...] = jnp.where(stat_lane < stat_out.shape[1] // 2, mean_own, spread_own)
    stats = remote(stat_out, stat_in, pair_sems.at[2], pair_sems.at[3], (e, other))
    stats.start()
    for copy in sends + forwards + downs + returns:
        copy.wait_send()
    stats.wait()
    mean_other = stat_in[:, 0:1]
    last = stat_in.shape[1]
    spread_other = stat_in[:, last - 1 : last]
    gap = mean_other - mean_own
    variance = (spread_own + spread_other + gap * gap * (half / 2)) / width
    gain = moe_gain[:, own_cols]
    out[...] = ((off - 0.5 * gap) * lax.rsqrt(variance + 1e-05) * gain).astype(BF16)


def per_device(
    tokens, old_state, w_query, w_forget, w_value, w_gate, lower_bound, head_gain, w_out,
    mix_gain, expert_gate, expert_up, expert_down, expert_ids, route_weight, moe_gain,
):
    rows, width = tokens.shape
    heads, state_width = old_state.shape[1:]
    hd = head_gain.shape[0]
    cols = w_query.shape[1]
    n = lax.axis_size("ep")
    half = width // lax.axis_size("tp")
    top = expert_ids.shape[1]
    capacity = max(2, 2 * top * rows // n)
    slots = -(-capacity // 8) * 8
    vmem = pl.BlockSpec(memory_space=pltpu.VMEM)
    hbm = pl.BlockSpec(memory_space=pltpu.MemorySpace.HBM)
    new_state, part = pl.pallas_call(
        mixer_kernel,
        out_shape=(
            jax.ShapeDtypeStruct(old_state.shape, F32),
            jax.ShapeDtypeStruct((rows, width), BF16),
        ),
        in_specs=[hbm] * 9,
        out_specs=(hbm, vmem),
        scratch_shapes=[
            pltpu.VMEM((rows, width), BF16),
            pltpu.VMEM((1, cols), F32),
            pltpu.VMEM((1, hd), F32),
            pltpu.VMEM((width, cols), BF16),
            pltpu.VMEM((width, cols), BF16),
            pltpu.VMEM((width, cols), BF16),
            pltpu.VMEM((width, cols), BF16),
            pltpu.VMEM((cols, width), BF16),
            pltpu.VMEM(old_state.shape, F32),
            pltpu.VMEM(old_state.shape, F32),
            pltpu.VMEM((2 * hd, state_width), BF16),
            pltpu.VMEM((rows, heads, 2 * hd), F32),
            pltpu.VMEM((rows, heads, 2 * hd), F32),
            pltpu.VMEM((rows, heads, 2 * hd), F32),
            pltpu.VMEM((rows, heads, hd), F32),
            pltpu.VMEM((rows, cols), F32),
            pltpu.SemaphoreType.DMA((9,)),
            pltpu.SemaphoreType.DMA((4,)),
        ],
        compiler_params=pltpu.CompilerParams(vmem_limit_bytes=GRANT),
        name="mixer",
    )(
        tokens, lower_bound.reshape(1, cols), head_gain.reshape(1, hd),
        old_state, w_query, w_forget, w_value, w_gate, w_out,
    )
    ff = expert_gate.shape[2]
    spare = slots - capacity
    wide = half
    if spare and capacity % spare == 0 and half % ((capacity // spare + 1) * 128) == 0:
        wide = half // (capacity // spare + 1) * (capacity // spare)
    slab = pltpu.VMEM((n, slots, wide), BF16)
    pieces = 4
    dma = pltpu.SemaphoreType.DMA
    next_tokens = pl.pallas_call(
        functools.partial(expert_kernel, capacity, n),
        out_shape=jax.ShapeDtypeStruct((rows, half), BF16),
        in_specs=[hbm] * 9,
        out_specs=vmem,
        scratch_shapes=[
            pltpu.VMEM((rows, width), BF16),
            pltpu.VMEM((rows, width), BF16),
            pltpu.VMEM((1, width), F32),
            pltpu.VMEM((top, rows), jnp.int32),
            pltpu.VMEM((top, rows), F32),
            pltpu.VMEM((1, width), F32),
            pltpu.VMEM((width, ff), BF16),
            pltpu.VMEM((width, ff), BF16),
            pltpu.VMEM((ff, width), BF16),
            pltpu.VMEM((rows, width), BF16),
            pltpu.VMEM((rows, width), F32),
            slab, slab, slab, slab, slab, slab, slab,
            pltpu.VMEM((rows, 128), F32),
            pltpu.VMEM((rows, 128), F32),
            dma((9,)), dma((4,)), dma((n,)), dma((n,)), dma((n,)), dma((n,)), dma((n,)), dma((n,)),
            dma((pieces,)), dma((pieces,)),
        ],
        compiler_params=pltpu.CompilerParams(
            collective_id=0, has_side_effects=True, vmem_limit_bytes=40 * 2**20
        ),
        name="experts",
    )(
        part, tokens, mix_gain.reshape(1, width), expert_ids.T, route_weight.T,
        moe_gain.reshape(1, width), expert_gate.reshape(width, ff), expert_up.reshape(width, ff),
        expert_down.reshape(ff, width),
    )
    return (next_tokens, new_state)


def solution(mesh):
    in_specs = (
        P("ep", None),
        P("ep", "tp", None),
        P(None, "tp"),
        P(None, "tp"),
        P(None, "tp"),
        P(None, "tp"),
        P("tp"),
        P(),
        P("tp", None),
        P(),
        P("ep", None, "tp"),
        P("ep", None, "tp"),
        P("ep", "tp", None),
        P("ep", None),
        P("ep", None),
        P(),
    )
    out_specs = (P("ep", "tp"), P("ep", "tp", None))
    return jax.shard_map(
        per_device, mesh=mesh, in_specs=in_specs, out_specs=out_specs, check_vma=False
    )
```
